1024 devices in a mesh: kv: 256 (over z, y, core), tp: 4 (over x).
Axes of the slice: x: 4, y: 8, z: 16, core: 2. Of those that a mesh axis runs over, the one named last changes fastest.
Arguments:
- queries: bfloat16 [65536, 4, 128], P('kv', 'tp'), may hold values from -6 to 6
- keys: bfloat16 [65536, 4, 128], P('kv', 'tp'), may hold values from -6 to 6
- values: bfloat16 [65536, 4, 128], P('kv', 'tp'), may hold values from -6 to 6
- attended: bfloat16 [65536, 4, 128], P('kv', 'tp'), may hold values from -6 to 6
- out_grad: bfloat16 [65536, 4, 128], P('kv', 'tp'), may hold values from -6 to 6
- log_sum: float32 [65536, 4], P('kv', 'tp'), may hold values from 2.5 to 4.5
- picked: int32 [512, 16], P('kv'), may hold values from -1 to 2047, as said below
- layer_input: bfloat16 [65536, 4096], P('kv'), may hold values from -0.09375 to 0.09375
Outputs:
- query_grad: float32 [65536, 4, 128], P('kv', 'tp')
- key_grad: float32 [65536, 4, 128], P('kv', 'tp')
- value_grad: float32 [65536, 4, 128], P('kv', 'tp')
- weight_grad: float32 [4096, 512], P('kv', 'tp')
The draws below stay inside these ranges and needn't reach their ends.
Inputs may be any that keep to these rules, and one draw needn't show every extreme that they name: Row r lists distinct key block numbers picked by query block r, followed by -1 to the end of the row; at least one entry is not -1, and at most 16 are. No picked block starts after the last position of its query block. With the span of a position being the position divided by 256 (rounded down), the span of every picked block is the query block's span or that span less 1, 2, 4, 8 and so on. The query blocks of one span pick at most 4 distinct blocks from any other single span.
All inputs are finite; a program needn't handle non-finite values.
Results may differ from the reference program's by a relative error of at most 0.004.
Values may be sent and summed in bfloat16 or wider, within the bound.
A program may use at most 32 MiB of HBM per device.

```python
import jax
import jax.numpy as jnp
from jax import lax

D = 4096
HEADS = 4
DH = 128
TOK_DEV = 256
QB = 128
KB = 32
MAXSEL = 16
PER_SPAN = 4
TOKENS = 65536
QBLOCKS = 512


def draw_picked(key, part):
    span_count = TOKENS // TOK_DEV
    span_blocks = TOK_DEV // KB
    query_count = TOK_DEV // QB
    levels = span_count.bit_length() - 1
    groups = levels + 1
    slot_total = groups * span_blocks
    allow_key = jax.random.fold_in(key, 11)
    score_key = jax.random.fold_in(key, 12)
    count_key_a = jax.random.fold_in(key, 13)
    count_key_b = jax.random.fold_in(key, 14)
    block_axis = jnp.arange(span_blocks, dtype=jnp.int32)
    allow_scores = jax.random.randint(allow_key, (span_count, groups, span_blocks), 0, 1 << 20, dtype=jnp.int32) * span_blocks + block_axis
    allow_rank = jnp.argsort(jnp.argsort(allow_scores, axis=-1), axis=-1)
    allowed = allow_rank < PER_SPAN
    span_index = jnp.arange(span_count, dtype=jnp.int32)[:, None, None, None]
    query_index = jnp.arange(query_count, dtype=jnp.int32)[None, :, None, None]
    group_index = jnp.arange(groups, dtype=jnp.int32)[None, None, :, None]
    block_index = block_axis[None, None, None, :]
    back_spans = jnp.where(group_index == 0, 0, jnp.left_shift(jnp.ones_like(group_index), jnp.maximum(group_index - 1, 0)))
    owner_span = span_index - back_spans
    own_usable = (group_index == 0) & (block_index * KB <= query_index * QB + QB - 1)
    far_usable = (group_index > 0) & (owner_span >= 0) & allowed[:, None, :, :]
    usable = own_usable | far_usable
    slot_index = group_index * span_blocks + block_index
    draw_scores = jax.random.randint(score_key, (span_count, query_count, groups, span_blocks), 0, 1 << 16, dtype=jnp.int32)
    unique = draw_scores * slot_total + slot_index
    masked = jnp.where(usable, unique, -1)
    group_best = jnp.max(masked, axis=-1, keepdims=True)
    last_query = query_index == query_count - 1
    forced = usable & (masked == group_best) | usable & last_query & (group_index == 1)
    ranked = jnp.where(usable, unique + jnp.where(forced, 1 << 28, 0), -1)
    half_most = MAXSEL // 2
    extra_picks = jax.random.randint(count_key_a, (span_count, query_count), 0, half_most + 1, dtype=jnp.int32) * jax.random.randint(count_key_b, (span_count, query_count), 0, half_most + 1, dtype=jnp.int32) // half_most
    usable_count = jnp.sum(usable.astype(jnp.int32), axis=(2, 3))
    forced_count = jnp.sum(forced.astype(jnp.int32), axis=(2, 3))
    last_row = (jnp.arange(query_count, dtype=jnp.int32) == query_count - 1)[None, :]
    wanted = jnp.where(last_row, MAXSEL, jnp.maximum(half_most + extra_picks, forced_count))
    pick_count = jnp.minimum(wanted, usable_count)
    flat_ranked = ranked.reshape(span_count, query_count, slot_total)
    top_values, top_slots = lax.top_k(flat_ranked, MAXSEL)
    chosen_group = top_slots // span_blocks
    chosen_block = top_slots % span_blocks
    chosen_back = jnp.where(chosen_group == 0, 0, jnp.left_shift(jnp.ones_like(chosen_group), jnp.maximum(chosen_group - 1, 0)))
    chosen_span = jnp.arange(span_count, dtype=jnp.int32)[:, None, None] - chosen_back
    chosen_ids = chosen_span * span_blocks + chosen_block
    position = jnp.arange(MAXSEL, dtype=jnp.int32)[None, None, :]
    chosen_ids = jnp.where(position < pick_count[:, :, None], chosen_ids, -1)
    return chosen_ids.reshape(span_count * query_count, MAXSEL).astype(jnp.int32)


def raised(array, own_key, source, target, shards_of, factor):
    def block_of(axis_at):
        return (jnp.arange(array.shape[axis_at]) // (array.shape[axis_at] // shards_of)).reshape((-1,) + (1,) * (array.ndim - 1 - axis_at))

    one_side = jax.random.permutation(own_key, shards_of)[block_of(target)]
    other_side = (block_of(target) + shards_of // 2) % shards_of
    return jnp.where((block_of(source) == one_side) | (block_of(source) == other_side), factor * array, array)


def level_of(stream_key, extent, split, smallest, high):
    gain, own = 1.0, jax.random.fold_in(stream_key, 6)
    for axis_at, blocks in split:
        draws = jnp.exp(jax.random.uniform(jax.random.fold_in(own, axis_at), (blocks,), jnp.float32, smallest / len(split), high / len(split)))
        gain = gain * jnp.repeat(draws, extent[axis_at] // blocks).reshape([-1 if axis == axis_at else 1 for axis in range(len(extent))])
    return gain


def gaussian(rng, dims, scale, bound, split=(), kind=jnp.bfloat16):
    entries = scale * jax.random.normal(rng, dims, jnp.float32)
    if split:
        entries = entries * level_of(rng, dims, split, -0.22, 0.18)
    return jnp.clip(entries, -bound, bound).astype(kind)


def heavy_noise(key, extent, spread, bound, cuts, heavy, kind=jnp.bfloat16):
    entries = spread * jax.random.normal(key, extent, jnp.float32)
    if cuts:
        entries = entries * level_of(key, extent, cuts, -0.22, 0.18)
    return jnp.clip(raised(entries, jax.random.fold_in(key, 3), *heavy), -bound, bound).astype(kind)


def setup_inputs(seed: int = 0) -> dict:
    arg_keys = jax.random.split(jax.random.key(seed), 9)
    queries = gaussian(arg_keys[0], (TOKENS, HEADS, DH), 1.0, 6.0, ((0, 256), (1, 4)))
    keys = gaussian(arg_keys[1], (TOKENS, HEADS, DH), 1.0, 6.0, ((0, 256), (1, 4)))
    values = gaussian(arg_keys[2], (TOKENS, HEADS, DH), 1.0, 6.0, ((0, 256), (1, 4)))
    attended = gaussian(arg_keys[3], (TOKENS, HEADS, DH), 1.0, 6.0, ((0, 256), (1, 4)))
    out_grad = gaussian(arg_keys[4], (TOKENS, HEADS, DH), 1.0, 6.0, ((0, 256), (1, 4)))
    log_sum = jnp.clip(2.5 + 2.0 * jax.random.uniform(arg_keys[5], (TOKENS, HEADS), jnp.float32) ** level_of(arg_keys[5], (TOKENS, HEADS), ((0, 256), (1, 4)), -0.2, 0.2), 2.5, 4.5)
    picked = draw_picked(jax.random.fold_in(arg_keys[8], 71), 0)
    layer_input = heavy_noise(arg_keys[7], (TOKENS, D), 0.004, 0.09375, ((0, 256),), (0, 1, 256, 6.0))
    return dict(queries=queries, keys=keys, values=values, attended=attended, out_grad=out_grad, log_sum=log_sum, picked=picked, layer_input=layer_input)


def reference(queries, keys, values, attended, out_grad, log_sum, picked, layer_input):
    score_scale = DH ** -0.5
    row_dots = jnp.sum(out_grad.astype(jnp.float32) * attended.astype(jnp.float32), axis=-1)
    key_offsets = jnp.arange(KB, dtype=jnp.int32)
    query_offsets = jnp.arange(QB, dtype=jnp.int32)

    def one_block(carry, block_index):
        key_sums, value_sums = carry
        listed = picked[block_index]
        listed_live = listed >= 0
        gather_rows = (jnp.where(listed_live, listed, 0)[:, None] * KB + key_offsets[None, :]).reshape(-1).astype(jnp.int32)
        key_live = jnp.repeat(listed_live, KB)
        first_query = (block_index * QB).astype(jnp.int32)
        query_pos = first_query + query_offsets
        pair_live = key_live[None, :] & (gather_rows[None, :] <= query_pos[:, None])
        query_rows = lax.dynamic_slice_in_dim(queries, first_query, QB, 0).astype(jnp.float32)
        grad_rows = lax.dynamic_slice_in_dim(out_grad, first_query, QB, 0).astype(jnp.float32)
        stored = lax.dynamic_slice_in_dim(log_sum, first_query, QB, 0)
        block_dots = lax.dynamic_slice_in_dim(row_dots, first_query, QB, 0)
        key_rows = keys[gather_rows].astype(jnp.float32)
        value_rows = values[gather_rows].astype(jnp.float32)
        scores = jnp.einsum("qhd,khd->hqk", query_rows, key_rows) * score_scale
        weights = jnp.where(pair_live[None], jnp.exp(scores - stored.T[:, :, None]), 0.0)
        slopes = jnp.einsum("qhd,khd->hqk", grad_rows, value_rows)
        score_grad = weights * (slopes - block_dots.T[:, :, None])
        weight_pairs = lax.optimization_barrier(weights.astype(jnp.bfloat16)).astype(jnp.float32)
        grad_pairs = lax.optimization_barrier(score_grad.astype(jnp.bfloat16)).astype(jnp.float32)
        query_grad = jnp.einsum("hqk,khd->qhd", grad_pairs, key_rows) * score_scale
        key_terms = jnp.einsum("hqk,qhd->khd", grad_pairs, query_rows) * score_scale
        value_terms = jnp.einsum("hqk,qhd->khd", weight_pairs, grad_rows)
        key_sums = key_sums.at[gather_rows].add(key_terms)
        value_sums = value_sums.at[gather_rows].add(value_terms)
        return (key_sums, value_sums), query_grad

    empty = jnp.zeros(keys.shape, jnp.float32)
    (key_grad, value_grad), query_grad = lax.scan(one_block, (empty, empty), jnp.arange(QBLOCKS, dtype=jnp.int32))
    query_grad = query_grad.reshape(TOKENS, HEADS, DH)
    value_round = value_grad.astype(jnp.bfloat16).reshape(TOKENS, HEADS * DH)
    weight_grad = lax.dot_general(layer_input, value_round, (((0,), (0,)), ((), ())), preferred_element_type=jnp.float32)
    return query_grad, key_grad, value_grad, weight_grad
```

```python
import jax
import jax.numpy as jnp
from jax import lax
from jax.experimental import pallas as pl
from jax.experimental.pallas import tpu as pltpu
from jax.sharding import PartitionSpec as P

MESH = pl.DeviceIdType.MESH
F32, BF16 = jnp.float32, jnp.bfloat16
NY, NZ = 8, 16
SPAN, DH, KB, D = 256, 128, 32, 4096
BLOCKS = SPAN // KB
SCALE = DH ** (-0.5)
DEAD = -1e30
YSTEP = {1: 1, 2: 2, 3: 4}
NT = (((1,), (1,)), ((), ()))
Y_ORDER = (4, 3, 5, 2, 6, 1, 7)
Z_ORDER = (8, 7, 9, 6, 10, 5, 11, 4, 12, 3, 13, 2, 14, 1, 15)


def dot(a, b):
    return jnp.dot(a, b, preferred_element_type=F32)


def main_kernel(
    picked_ref, q_hbm, k_hbm, v_hbm, o_hbm, g_hbm, ls_hbm, x_hbm,
    dq_ref, dk_ref, dv_ref, w_ref,
    qd_own, aux_own, kk, vv, oo, ls, kt, qd, aux, pbuf, sbuf, dqt, dq4,
    ret_out, ret_in, xx, xt, xr, vb, vm, pf, pb, yb, sf, sb, zb,
    lsem, qsend, qrecv, rsend, rrecv, xsem, vsem, ysend, yrecv, zsend, zrecv, late,
):
    me = lax.axis_index("kv")
    z, y, c = me // (2 * NY), (me // 2) % NY, me % 2

    def dev(zz, yy, cc):
        return zz * (2 * NY) + yy * 2 + cc

    mate = dev(z, y, 1 - c)
    cross = dev(z, (y + 7 + 2 * c) % NY, 1 - c)
    ypeer = {d: dev(z, (y + d) % NY, c) for d in range(1, NY)}
    zpeer = {d: dev((z + d) % NZ, y, c) for d in range(1, NZ)}
    partners = [mate, cross, *ypeer.values(), *zpeer.values()]
    beside_first = (me != 0) & ((me == 1) | (me == dev(0, NY - 1, 1)) | ((z == 0) & (c == 0)) | ((y == 0) & (c == 0)))

    def remote(src, dst, send, recv, target):
        return pltpu.make_async_remote_copy(
            src_ref=src, dst_ref=dst, send_sem=send, recv_sem=recv, device_id={"kv": target}, device_id_type=MESH
        )

    barrier = pltpu.get_barrier_semaphore()

    @pl.when(me != 0)
    def _():
        for p in partners:
            pl.semaphore_signal(barrier, inc=1, device_id={"kv": p}, device_id_type=MESH)

    loads = [
        pltpu.make_async_copy(q_hbm, qd_own.at[pl.ds(0, SPAN)], lsem.at[0]),
        pltpu.make_async_copy(g_hbm, qd_own.at[pl.ds(SPAN, SPAN)], lsem.at[1]),
        pltpu.make_async_copy(o_hbm, oo, lsem.at[2]),
        pltpu.make_async_copy(ls_hbm, ls, lsem.at[3]),
        pltpu.make_async_copy(k_hbm, kk, lsem.at[4]),
        pltpu.make_async_copy(v_hbm, vv, lsem.at[5]),
        pltpu.make_async_copy(x_hbm, xx, lsem.at[6]),
    ]
    for load in loads:
        load.start()

    picked = picked_ref[...]
    back = me - picked // BLOCKS
    group = jnp.zeros_like(picked)
    for level in range(8):
        group = group + (back >= (1 << level)).astype(jnp.int32)
    bit = (group - 1) * BLOCKS + picked % BLOCKS
    live = picked >= 0
    lane = lax.broadcasted_iota(jnp.int32, (1, SPAN), 1)

    def word_row(low, high):
        inside = live & (bit >= low) & (bit < high)
        value = jnp.where(inside, jnp.left_shift(jnp.ones_like(bit), jnp.where(inside, bit - low, 0)), 0)
        total = jnp.sum(value.astype(F32), axis=1, keepdims=True)
        return jnp.where(lane < SPAN // 2, total[0:1, :], total[1:2, :])

    own_word = word_row(-BLOCKS, 0)
    words = [word_row(0, 24), word_row(24, 48), word_row(48, 64)]
    for load in loads[:4]:
        load.wait()
    prod = qd_own[SPAN:, :].astype(F32) * oo[...].astype(F32)
    dots = jnp.sum(prod.T, axis=0, keepdims=True)
    aux_own[0:1, :] = ls[...]
    aux_own[1:2, :] = dots
    for i in range(3):
        aux_own[2 + i : 3 + i, :] = words[i]
    aux_own[5:8, :] = jnp.zeros((3, SPAN), F32)

    @pl.when(me == 0)
    def _():
        pl.semaphore_wait(barrier, len(partners))
        for p in partners:
            pl.semaphore_signal(late, inc=1, device_id={"kv": p}, device_id_type=MESH)

    @pl.when(me != 0)
    def _():
        pl.semaphore_wait(barrier, len(partners) - beside_first.astype(jnp.int32))

    def part(level, j, source, target):
        if j == 0:
            src = aux_own if source is None else aux.at[source]
            dst = aux.at[level]
        else:
            rows = pl.ds((j - 1) * SPAN, SPAN)
            src = qd_own.at[rows] if source is None else qd.at[source, rows]
            dst = qd.at[level, rows]
        return remote(src, dst, qsend.at[level, j], qrecv.at[level, j], target)

    def send(level, source, target):
        for j in range(3):
            part(level, j, source, target).start()

    down = {d: dev(z, (y + NY - d) % NY, c) for d in (1, 2, 4)}
    target = {0: jnp.where(c == 1, mate, cross), 4: dev(z - 1, y, c), 5: dev(z - 1, y, c), 6: dev(z - 2, y, c), 7: dev(z - 8, y, c)}
    owns = {0: (c == 1) | (y >= 1), 4: z >= 1, 7: z >= 8}
    sends = {0: owns[0] | (z < NZ - 1), 4: z >= 1, 5: (z >= 1) & (z < NZ - 1), 6: (z >= 2) & (z < NZ - 2), 7: z >= 8}
    origin = {0: jnp.where(c == 0, mate, cross), 4: dev(z + 1, y, c), 5: dev(z + 2, y, c), 6: dev(z + 4, y, c), 7: dev(z + 8, y, c)}
    gets = {0: (c == 0) | (y < NY - 1) | (z < NZ - 1), 4: z < NZ - 1, 5: z < NZ - 2, 6: z < NZ - 4, 7: z < NZ - 8}
    for level, d in YSTEP.items():
        target[level] = down[d]
        owns[level] = y >= d
        sends[level] = owns[level] | (z < NZ - 1)
        origin[level] = ypeer[d]
        gets[level] = (y + d < NY) | (z < NZ - 1)

    def begin(level, now):
        pl.when(owns[level] & now(target[level]))(lambda: send(level, None, target[level]))

    for level in (4, 7, 3, 2, 1, 0):
        begin(level, lambda t: t != 0)

    for load in loads[4:6]:
        load.wait()
    kt[...] = kk[...].T

    def attend(queries, grads, aux_view, row, shift, own):
        scores = lax.dot_general(kk[...], queries, NT, preferred_element_type=F32)
        slopes = lax.dot_general(vv[...], grads, NT, preferred_element_type=F32)
        info = aux_view[...]
        stored, block_dots = info[0:1, :], info[1:2, :]
        word = (own_word if own else info[row : row + 1, :]).astype(jnp.int32)
        for b in range(BLOCKS):
            rows = slice(b * KB, (b + 1) * KB)
            shifted = jnp.right_shift(word, shift + b)
            bias = jnp.where(shifted % 2 == 1, -stored, DEAD)
            weights = jnp.exp(scores[rows] * SCALE + bias)
            if own:
                key_at = b * KB + lax.broadcasted_iota(jnp.int32, (KB, SPAN), 0)
                query_at = lax.broadcasted_iota(jnp.int32, (KB, SPAN), 1)
                weights = jnp.where(key_at <= query_at, weights, 0.0)
            pbuf[rows, :] = weights.astype(BF16)
            sbuf[rows, :] = (weights * (slopes[rows] - block_dots)).astype(BF16)
        value_part = dot(pbuf[...], grads)
        key_part = dot(sbuf[...], queries)
        if own:
            dv_ref[...] = value_part
            dk_ref[...] = key_part
        else:
            dv_ref[...] += value_part
            dk_ref[...] += key_part
        return dot(kt[...], sbuf[...])

    dqt[...] = attend(qd_own[:SPAN, :], qd_own[SPAN:, :], aux_own, 0, 0, True)

    loads[6].wait()

    @pl.loop(0, NZ)
    def _(zz):
        cols = pl.ds(pl.multiple_of(zz * SPAN, SPAN), SPAN)
        turned = xx[:, cols].T
        place = pl.ds(pl.multiple_of(zz * 16, 16), 16)
        for yy in range(NY):
            for cc in range(2):
                xt[cc, yy, place, :] = turned[yy * 32 + cc * 16 : yy * 32 + cc * 16 + 16, :]

    x_copy = remote(xt.at[1 - c], xr, xsem.at[0], xsem.at[1], mate)
    pl.when(mate != 0)(x_copy.start)

    @pl.when(gets[4])
    def _():
        for j in range(3):
            part(4, j, None, target[4]).wait_recv()
            pl.when((z >= 1) & (target[5] != 0))(lambda: part(5, j, 4, target[5]).start())

    for level in (3, 2, 1, 0):
        pl.when(jnp.logical_not(owns[level]) & gets[4])(lambda: send(level, 4, target[level]))

    @pl.when(gets[5])
    def _():
        for j in range(3):
            part(5, j, None, target[5]).wait_recv()
            pl.when((z >= 2) & (target[6] != 0))(lambda: part(6, j, 5, target[6]).start())

    def give_back(level):
        return remote(ret_out.at[level], ret_in.at[level], rsend.at[level], rrecv.at[level], origin[level])

    def process(level, wait):
        if wait:
            for j in range(3):
                part(level, j, None, target[level]).wait_recv()
        got = attend(qd[level, :SPAN, :], qd[level, SPAN:, :], aux.at[level], 2 + level // 3, level % 3 * BLOCKS, False)
        if level == 4:
            dq4[...] = got
        else:
            ret_out[level] = got.astype(BF16)
            give_back(level).start()

    pl.when(gets[4])(lambda: process(4, False))
    for level in (0, 1, 2, 3):
        pl.when(gets[level])(lambda: process(level, True))

    @pl.when(beside_first)
    def _():
        pl.semaphore_wait(late, 1)
        for level in (4, 7, 3, 2, 1, 0):
            begin(level, lambda t: t == 0)
        pl.when(me == dev(1, 0, 0))(lambda: send(5, 4, 0))
        pl.when(me == dev(2, 0, 0))(lambda: send(6, 5, 0))
        pl.when(mate == 0)(x_copy.start)

    pl.when(gets[5])(lambda: process(5, False))
    for level in (6, 7):
        pl.when(gets[level])(lambda: process(level, True))

    vb[...] = dv_ref[...].astype(BF16)
    v_copy = remote(vb, vm, vsem.at[0], vsem.at[1], mate)
    v_copy.start()
    for d in range(NY):
        at = (y + d) % NY
        pf[d] = dot(xt[c, at], vb[...])
    x_copy.wait_recv()
    v_copy.wait_recv()

    def y_copy(d):
        return remote(pb.at[d], yb.at[d], ysend.at[d], yrecv.at[d], ypeer[d])

    for d in Y_ORDER:
        at = (y + d) % NY
        pb[d] = (pf[d] + dot(xr[at], vm[...])).astype(BF16)
        y_copy(d).start()
    total = pf[0] + dot(xr[y], vm[...])

    for level in (0, 1, 2, 3):
        @pl.when(sends[level])
        def _(level=level):
            give_back(level).wait_recv()

            @pl.when(owns[level])
            def _():
                dqt[...] += ret_in[level].astype(F32)

            @pl.when(jnp.logical_not(owns[level]))
            def _():
                dq4[...] += ret_in[level].astype(F32)

    @pl.when(gets[4])
    def _():
        ret_out[4] = dq4[...].astype(BF16)
        give_back(4).start()

    for d in Y_ORDER:
        y_copy(d).wait_recv()
        total = total + yb[d].astype(F32)
    for zz in range(NZ):
        rows = total[zz * 16 : zz * 16 + 16, :]
        sf[zz] = rows
        sb[zz] = rows.astype(BF16)

    def z_copy(d):
        return remote(sb.at[(z + d) % NZ], zb.at[d], zsend.at[d], zrecv.at[d], zpeer[d])

    for d in Z_ORDER:
        z_copy(d).start()

    for level, there in ((4, z >= 1), (5, z >= 2), (6, z >= 4), (7, z >= 8)):
        @pl.when(there)
        def _(level=level):
            give_back(level).wait_recv()
            dqt[...] += ret_in[level].astype(F32)

    dq_ref[...] = dqt[...].T

    out = sf[z]
    for d in Z_ORDER:
        z_copy(d).wait_recv()
        out = out + zb[d].astype(F32)
    w_ref[...] = out

    for level in range(8):
        @pl.when(sends[level])
        def _(level=level):
            for j in range(3):
                part(level, j, None, target[level]).wait_send()

        pl.when(gets[level])(give_back(level).wait_send)
    x_copy.wait_send()
    v_copy.wait_send()
    for d in Y_ORDER:
        y_copy(d).wait_send()
    for d in Z_ORDER:
        z_copy(d).wait_send()


def last_kernel(dq_in, dk_in, dv_in, w_in, dq_ref, dk_ref, dv_ref, w_ref):
    dq_ref[...] = dq_in[...] * SCALE
    dk_ref[...] = dk_in[...] * SCALE
    dv_ref[...] = dv_in[...]
    w_ref[...] = w_in[...]


def per_device(queries, keys, values, attended, out_grad, log_sum, picked, layer_input):
    flat = [a.reshape(SPAN, DH) for a in (queries, keys, values, attended, out_grad)]
    stored = log_sum.reshape(1, SPAN)
    hbm = pl.BlockSpec(memory_space=pl.ANY)
    vmem = pl.BlockSpec(memory_space=pltpu.VMEM)
    outs = [jax.ShapeDtypeStruct((SPAN, DH), F32)] * 3 + [jax.ShapeDtypeStruct((16, DH), F32)]
    sem = pltpu.SemaphoreType.DMA
    scratch = [
        pltpu.VMEM((2 * SPAN, DH), BF16),
        pltpu.VMEM((8, SPAN), F32),
        pltpu.VMEM((SPAN, DH), BF16),
        pltpu.VMEM((SPAN, DH), BF16),
        pltpu.VMEM((SPAN, DH), BF16),
        pltpu.VMEM((1, SPAN), F32),
        pltpu.VMEM((DH, SPAN), BF16),
        pltpu.VMEM((8, 2 * SPAN, DH), BF16),
        pltpu.VMEM((8, 8, SPAN), F32),
        pltpu.VMEM((SPAN, SPAN), BF16),
        pltpu.VMEM((SPAN, SPAN), BF16),
        pltpu.VMEM((DH, SPAN), F32),
        pltpu.VMEM((DH, SPAN), F32),
        pltpu.VMEM((8, DH, SPAN), BF16),
        pltpu.VMEM((8, DH, SPAN), BF16),
        pltpu.VMEM((SPAN, D), BF16),
        pltpu.VMEM((2, NY, SPAN, SPAN), BF16),
        pltpu.VMEM((NY, SPAN, SPAN), BF16),
        pltpu.VMEM((SPAN, DH), BF16),
        pltpu.VMEM((SPAN, DH), BF16),
        pltpu.VMEM((NY, SPAN, DH), F32),
        pltpu.VMEM((NY, SPAN, DH), BF16),
        pltpu.VMEM((NY, SPAN, DH), BF16),
        pltpu.VMEM((NZ, 16, DH), F32),
        pltpu.VMEM((NZ, 16, DH), BF16),
        pltpu.VMEM((NZ, 16, DH), BF16),
        sem((7,)), sem((8, 3)), sem((8, 3)), sem((8,)), sem((8,)), sem((2,)), sem((2,)),
        sem((NY,)), sem((NY,)), sem((NZ,)), sem((NZ,)), pltpu.SemaphoreType.REGULAR,
    ]
    got = pl.pallas_call(
        main_kernel,
        out_shape=outs,
        in_specs=[vmem] + [hbm] * 7,
        out_specs=[vmem] * 4,
        scratch_shapes=scratch,
        compiler_params=pltpu.CompilerParams(collective_id=0, has_side_effects=True),
        name="exchange",
    )(picked, *flat, stored, layer_input)
    got = pl.pallas_call(last_kernel, out_shape=outs, in_specs=[vmem] * 4, out_specs=[vmem] * 4, name="finish")(*got)
    return tuple(a.reshape(SPAN, 1, DH) for a in got[:3]) + (got[3],)


def solution(mesh):
    return jax.shard_map(
        per_device,
        mesh=mesh,
        in_specs=(P("kv", "tp", None),) * 5 + (P("kv", "tp"), P("kv", None), P("kv", None)),
        out_specs=(P("kv", "tp", None),) * 3 + (P("kv", "tp"),),
        check_vma=False,
    )
```
